128 devices in a mesh: fs: 32 (over z, y, core), tp: 4 (over x).
Axes of the slice: x: 4, y: 4, z: 4, core: 2. Of those that a mesh axis runs over, the one named last changes fastest.
Arguments:
- normed_input: bfloat16 [147456, 2048], P('fs'), may hold values from -12 to 12
- query_latent_cotangent: bfloat16 [147456, 768], P('fs', 'tp'), may hold values from -0.015625 to 0.015625
- key_value_latent_cotangent: bfloat16 [147456, 512], P('fs', 'tp'), may hold values from -0.015625 to 0.015625
- row_factor: bfloat16 [2048, 256], P('fs'), may hold values from -0.25 to 0.25
- query_down_weight: float32 [2048, 768], P('fs', 'tp'), may hold values from -6 to 6
- key_value_down_weight: float32 [2048, 512], P('fs', 'tp'), may hold values from -6 to 6
- query_first_moment: float32 [256, 768], P('fs', 'tp'), may hold values from -6 to 6
- key_value_first_moment: float32 [256, 512], P('fs', 'tp'), may hold values from -6 to 6
- query_second: float32 [256, 768], P('fs', 'tp'), may hold values from 0.5 to 2000
- latent_second: float32 [256, 512], P('fs', 'tp'), may hold values from 0.5 to 2000
Outputs:
- query_new: float32 [2048, 768], P('fs', 'tp')
- latent_new: float32 [2048, 512], P('fs', 'tp')
- query_step: float32 [2048, 768], P('fs', 'tp')
- latent_step: float32 [2048, 512], P('fs', 'tp')
- query_copy: bfloat16 [2048, 768], P(None, 'tp')
- latent_copy: bfloat16 [2048, 512], P(None, 'tp')
- query_first_new: float32 [256, 768], P('fs', 'tp')
- latent_first_new: float32 [256, 512], P('fs', 'tp')
- query_second_new: float32 [256, 768], P('fs', 'tp')
- latent_second_new: float32 [256, 512], P('fs', 'tp')
The draws below stay inside these ranges and needn't reach their ends.
All inputs are finite; a program needn't handle non-finite values.
Results may differ from the reference program's by a relative error of at most 0.006.
Values may be sent and summed in bfloat16 or wider, within the bound.
No kernel may reach another device: no remote copies, remote signals or barrier semaphores. Data moves between devices by JAX's collectives and lax.ppermute only.
A program may use at most 64 MiB of HBM per device.

```python
import jax
import jax.numpy as jnp
from jax import lax

MODEL_WIDTH = 2048
QUERY_LATENT = 768
KEY_VALUE_LATENT = 512
PROJECTION_RANK = 256
TOKEN_TOTAL = 147456


def second_moment_estimate(key, rows, cols):
    key_two = jax.random.fold_in(key, 1)
    row_index = jnp.arange(rows, dtype=jnp.float32) / max(rows - 1, 1)
    col_index = jnp.arange(cols, dtype=jnp.float32) / max(cols - 1, 1)
    col_scale = 10.0 ** col_index
    row_scale = 100.0 ** row_index
    jitter = jnp.exp(jax.random.uniform(key_two, (rows, cols), jnp.float32, -0.69, 0.69))
    return row_scale[:, None] * col_scale[None, :] * jitter


def draw_query_second(key, part):
    return second_moment_estimate(jax.random.fold_in(key, 11), PROJECTION_RANK, QUERY_LATENT)


def draw_latent_second(key, part):
    return second_moment_estimate(jax.random.fold_in(key, 12), PROJECTION_RANK, KEY_VALUE_LATENT)


def spiked(values, key, source, target, blocks, factor):
    owner, partner = [(jnp.arange(values.shape[position]) // (values.shape[position] // blocks)).reshape([-1 if axis == position else 1 for axis in range(values.ndim)]) for position in (source, target)]
    chosen = jax.random.permutation(key, blocks)[partner]
    strong = (owner == chosen) | (owner == (partner + blocks // 2) % blocks)
    return jnp.where(strong, factor * values, values)


def block_levels(key, shape, shards, low, top_value):
    factor_of, own = 1.0, jax.random.fold_in(key, 6)
    for dim, parts in shards:
        draws = jnp.exp(jax.random.uniform(jax.random.fold_in(own, dim), (parts,), jnp.float32, low / len(shards), top_value / len(shards)))
        factor_of = factor_of * jnp.repeat(draws, shape[dim] // parts).reshape([-1 if axis == dim else 1 for axis in range(len(shape))])
    return factor_of


def centred(key, shape, scale, bound, cuts=(), kind=jnp.bfloat16):
    result = jax.random.normal(key, shape, jnp.float32) * scale
    if len(cuts) > 0:
        result = block_levels(key, shape, cuts, -0.22, 0.18) * result
    return jnp.clip(result, min=-bound, max=bound).astype(kind)


def gaussian_with(own_key, dims, scale, limit, pieces, heavy, kind=jnp.bfloat16):
    result = scale * jax.random.normal(own_key, dims, jnp.float32)
    if pieces:
        result = result * block_levels(own_key, dims, pieces, -0.22, 0.18)
    return jnp.clip(spiked(result, jax.random.fold_in(own_key, 3), *heavy), -limit, limit).astype(kind)


def setup_inputs(seed: int = 0) -> dict:
    keys = jax.random.split(jax.random.key(seed), 11)
    return {
        "normed_input": gaussian_with(keys[0], (TOKEN_TOTAL, MODEL_WIDTH), 1.0, 12.0, ((0, 32),), (0, 1, 32, 2.75)),
        "query_latent_cotangent": centred(keys[1], (TOKEN_TOTAL, QUERY_LATENT), (TOKEN_TOTAL ** -0.5), 0.015625, ((0, 32), (1, 4))),
        "key_value_latent_cotangent": centred(keys[2], (TOKEN_TOTAL, KEY_VALUE_LATENT), (TOKEN_TOTAL ** -0.5), 0.015625, ((0, 32), (1, 4))),
        "row_factor": gaussian_with(keys[3], (MODEL_WIDTH, PROJECTION_RANK), MODEL_WIDTH ** -0.5, 0.25, ((0, 32),), (0, 1, 32, 2.75)),
        "query_down_weight": centred(keys[4], (MODEL_WIDTH, QUERY_LATENT), 1.0, 6.0, ((0, 32), (1, 4)), jnp.float32),
        "key_value_down_weight": centred(keys[5], (MODEL_WIDTH, KEY_VALUE_LATENT), 1.0, 6.0, ((0, 32), (1, 4)), jnp.float32),
        "query_first_moment": centred(keys[6], (PROJECTION_RANK, QUERY_LATENT), 1.0, 6.0, ((0, 32), (1, 4)), jnp.float32),
        "key_value_first_moment": centred(keys[7], (PROJECTION_RANK, KEY_VALUE_LATENT), 1.0, 6.0, ((0, 32), (1, 4)), jnp.float32),
        "query_second": draw_query_second(jax.random.fold_in(keys[10], 71), 0),
        "latent_second": draw_latent_second(jax.random.fold_in(keys[10], 71), 0),
    }


def token_sum(left, right):
    return lax.dot_general(left, right, (((0,), (0,)), ((), ())), preferred_element_type=jnp.float32)

def update_one(gradient, factor32, weight, first, second):
    projected = jnp.dot(factor32.T, gradient, precision=lax.Precision.HIGHEST)
    first_new = 0.8 * first + 0.2 * projected
    second_new = 0.9 * second + 0.1 * projected * projected
    direction = first_new / (jnp.sqrt(second_new) + 1e-08)
    count = direction.shape[0] * direction.shape[1]
    scale = 0.5 * jnp.sqrt(jnp.float32(count)) / jnp.sqrt(jnp.sum(direction * direction) + 1e-06)
    step = jnp.dot(factor32, scale * direction, precision=lax.Precision.HIGHEST)
    weight_new = weight - step
    return (weight_new, step, weight_new.astype(jnp.bfloat16), first_new, second_new)

def reference(normed_input, query_latent_cotangent, key_value_latent_cotangent, row_factor, query_down_weight, key_value_down_weight, query_first_moment, key_value_first_moment, query_second, latent_second):
    factor32 = row_factor.astype(jnp.float32)
    grad_q = token_sum(normed_input, query_latent_cotangent)
    grad_kv = token_sum(normed_input, key_value_latent_cotangent)
    qn, qs, qc, qf, qv = update_one(grad_q, factor32, query_down_weight, query_first_moment, query_second)
    kn, ks, kc, kf, kv = update_one(grad_kv, factor32, key_value_down_weight, key_value_first_moment, latent_second)
    return (qn, kn, qs, ks, qc, kc, qf, kf, qv, kv)
```

```python
import jax
import jax.numpy as jnp
from jax import lax
from jax.experimental import pallas as pl
from jax.experimental.pallas import tpu as pltpu
from jax.sharding import Mesh
from jax.sharding import PartitionSpec as P


FS = ("z", "y", "core")
ZY = ("z", "y")
BF16 = jnp.bfloat16
F32 = jnp.float32
VMEM = pl.BlockSpec(memory_space=pltpu.MemorySpace.VMEM)
SMEM = pl.BlockSpec(memory_space=pltpu.MemorySpace.SMEM)
HBM = pl.BlockSpec(memory_space=pltpu.MemorySpace.HBM)
PLACES = {id(VMEM): pltpu.MemorySpace.VMEM, id(HBM): pltpu.MemorySpace.HBM}


def near(dims, kind=F32):
    return pltpu.MemorySpace.VMEM(dims, kind)


def far(dims, kind=F32):
    return jax.ShapeDtypeStruct(dims, kind)


def run(kernel, specs, operands, out, scratch=(), flops=0, limit=8):
    operands = [
        pltpu.with_memory_space_constraint(o, PLACES[id(s)]) if id(s) in PLACES else o
        for s, o in zip(specs, operands)
    ]
    return pl.pallas_call(
        kernel,
        in_specs=list(specs),
        out_specs=[VMEM] * len(out),
        out_shape=list(out),
        scratch_shapes=list(scratch),
        compiler_params=pltpu.CompilerParams(vmem_limit_bytes=limit * 1024 * 1024),
        cost_estimate=pl.CostEstimate(flops=flops, bytes_accessed=0, transcendentals=0),
    )(*operands)


def exchange(tiles, axis):
    return lax.all_to_all(tiles, axis, split_axis=0, concat_axis=0, tiled=True)


def swapped(array, axis, bit):
    count = lax.axis_size(axis)
    return lax.ppermute(array, axis, [(i, i ^ bit) for i in range(count)])


def shifted(array, axis):
    count = lax.axis_size(axis)
    tiles = [array]
    for k in range(1, count):
        tiles.append(lax.ppermute(array, axis, [(i, (i + k) % count) for i in range(count)]))
    return tiles


def fetch(pairs, sems):
    copies = [pltpu.make_async_copy(a, b, sems.at[i]) for i, (a, b) in enumerate(pairs)]
    for copy in copies:
        copy.start()
    for copy in copies:
        copy.wait()


LANES = 128


def spread_kernel(factor_ref, q_ref, kv_ref, factor_out, weight_out, factor_buf, q_buf, kv_buf, sems):
    fetch(((factor_ref, factor_buf), (q_ref, q_buf), (kv_ref, kv_buf)), sems)
    rows = q_ref.shape[0]
    factor = factor_buf[...]
    q, kv = q_buf[...].astype(BF16), kv_buf[...].astype(BF16)
    for i in range(factor_out.shape[0]):
        factor_out[i] = factor
    weight_out[:rows, :LANES] = q[:, :LANES]
    weight_out[:rows, LANES:] = kv
    quarter = rows // 4
    rest = q[:, LANES:]
    for g in range(4):
        weight_out[rows:, 64 * g : 64 * (g + 1)] = rest[quarter * g : quarter * (g + 1)]


def spread(factor, q, kv, count):
    rows = factor.shape[0]
    return run(
        spread_kernel,
        [HBM] * 3,
        (factor, q, kv),
        [near((count, *factor.shape), BF16), near((rows + rows // 4, 2 * LANES), BF16)],
        [
            pltpu.VMEM(factor.shape, BF16),
            pltpu.VMEM(q.shape, F32),
            pltpu.VMEM(kv.shape, F32),
            pltpu.SemaphoreType.DMA((3,)),
        ],
    )


def stack_kernel(*refs):
    for i, ref in enumerate(refs[:-1]):
        refs[-1][i] = ref[...]


def stacked(tiles):
    return run(
        stack_kernel, [VMEM] * len(tiles), tiles, [near((len(tiles), *tiles[0].shape), BF16)]
    )[0]


def gradient_kernel(block, depth):
    def kernel(q_ref, kv_ref, x_ref, out_ref, q_buf, kv_buf, x_buf, sems):
        tokens = x_ref.shape[0]
        steps = tokens // block

        def copies(k):
            at, slot = pl.ds(k * block, block), k % depth
            return (
                pltpu.make_async_copy(q_ref.at[:, at], q_buf.at[slot], sems.at[slot, 0]),
                pltpu.make_async_copy(kv_ref.at[at, :], kv_buf.at[slot], sems.at[slot, 1]),
                pltpu.make_async_copy(x_ref.at[at, :], x_buf.at[slot], sems.at[slot, 2]),
            )

        for k in range(depth):
            for copy in copies(k):
                copy.start()
        for k in range(steps):
            slot = k % depth
            for copy in copies(k):
                copy.wait()
            left = jnp.concatenate([q_buf[slot], kv_buf[slot].T], axis=0)
            piece = jnp.dot(left, x_buf[slot], preferred_element_type=F32)
            if k == 0:
                out_ref[...] = piece
            else:
                out_ref[...] += piece
            if k + depth < steps:
                for copy in copies(k + depth):
                    copy.start()

    return kernel


def gradients(q_turned, kv, x, block=512, depth=4):
    q_width, kv_width = q_turned.shape[0], kv.shape[1]
    width = q_width + kv_width
    tokens, model = x.shape
    return run(
        gradient_kernel(block, depth),
        [HBM] * 3,
        (q_turned, kv, x),
        [near((width, model))],
        [
            pltpu.VMEM((depth, q_width, block), BF16),
            pltpu.VMEM((depth, block, kv_width), BF16),
            pltpu.VMEM((depth, block, model), BF16),
            pltpu.SemaphoreType.DMA((depth, 3)),
        ],
        2 * width * tokens * model,
        20,
    )[0]


def assemble(place_ref, mine_ref, other_ref, factor_ref):
    core = place_ref[2]
    for i in range(mine_ref.shape[0]):
        factor_ref[i, core] = mine_ref[i]
        factor_ref[i, 1 - core] = other_ref[i]
    count, pair, rows, rank = factor_ref.shape
    return factor_ref[...].reshape(count * pair * rows, rank)


def whole_factor(mine):
    count, rows, rank = mine.shape
    return pltpu.VMEM((count, 2, rows, rank), BF16)


def project_kernel(place_ref, mine_ref, other_ref, grad_ref, out_ref, factor_ref):
    factor = assemble(place_ref, mine_ref, other_ref, factor_ref)
    grad = grad_ref[...]
    upper = grad.astype(BF16)
    lower = (grad - upper.astype(F32)).astype(BF16)
    turned = jnp.dot(upper, factor, preferred_element_type=F32) + jnp.dot(
        lower, factor, preferred_element_type=F32
    )
    out_ref[...] = turned.T.astype(BF16)


def project(place, mine, other, grad):
    return run(
        project_kernel,
        [SMEM, VMEM, VMEM, VMEM],
        (place, mine, other, grad),
        [near((mine.shape[2], grad.shape[0]), BF16)],
        [whole_factor(mine)],
    )[0]


def updated(parts_ref, qm_ref, km_ref, qs_ref, ks_ref):
    projected = jnp.sum(parts_ref[...].astype(F32), axis=0)
    q_width = qm_ref.shape[1]
    for value, first_ref, second_ref in (
        (projected[:, :q_width], qm_ref, qs_ref),
        (projected[:, q_width:], km_ref, ks_ref),
    ):
        first = 0.8 * first_ref[...] + 0.2 * value
        second = 0.9 * second_ref[...] + 0.1 * value * value
        yield first, second


def direction_kernel(parts_ref, qm_ref, km_ref, qs_ref, ks_ref, dir_ref):
    at = 0
    for first, second in updated(parts_ref, qm_ref, km_ref, qs_ref, ks_ref):
        direction = (first / (jnp.sqrt(second) + 1e-08)).astype(BF16)
        width = direction.shape[1]
        for i in range(dir_ref.shape[0]):
            dir_ref[i, :, at : at + width] = direction
        at += width


def direction_tiles(parts, moments):
    return run(direction_kernel, [VMEM] * 5, (parts, *moments), [near(parts.shape, BF16)])[0]


def keep_kernel(parts_ref, qm_ref, km_ref, qs_ref, ks_ref, qm_out, km_out, qs_out, ks_out):
    outs = ((qm_out, qs_out), (km_out, ks_out))
    values = updated(parts_ref, qm_ref, km_ref, qs_ref, ks_ref)
    for (first, second), (first_out, second_out) in zip(values, outs):
        first_out[...] = first
        second_out[...] = second


def keep(parts, moments):
    return run(keep_kernel, [VMEM] * 5, (parts, *moments), [far(m.shape) for m in moments])


def stats_kernel(q_width):
    def kernel(dir_ref, out_ref):
        values = dir_ref[...].astype(F32)
        squares = jnp.sum(values * values, axis=0, keepdims=True)
        out_ref[0:1, :] = jnp.broadcast_to(jnp.sum(squares[:, :q_width], axis=1, keepdims=True), (1, 128))
        out_ref[1:2, :] = jnp.broadcast_to(jnp.sum(squares[:, q_width:], axis=1, keepdims=True), (1, 128))
        out_ref[2:, :] = jnp.zeros((6, 128), F32)

    return kernel


def stats(directions, q_width):
    return run(stats_kernel(q_width), [VMEM], (directions,), [near((8, 128))])[0]


def weights_kernel(place_ref, *refs):
    tiles, (q_ref, kv_ref, first_ref, rest_ref) = refs[:-4], refs[-4:]
    z, y, core = place_ref[0], place_ref[1], place_ref[2]
    count = len(tiles) // 2
    rows = first_ref.shape[3]
    quarter = rows // 4
    for t, tile in enumerate(tiles):
        c = core if t < count else 1 - core
        zi = lax.rem(z + count - t % count, count)
        for k in range(count):
            yi = lax.rem(y + count - k, count)
            first_ref[zi, yi, c] = tile[k, :rows, :LANES]
            kv_ref[zi, yi, c] = tile[k, :rows, LANES:]
            for g in range(4):
                rest_ref[zi, yi, c, quarter * g : quarter * (g + 1), :64] = tile[
                    k, rows:, 64 * g : 64 * (g + 1)
                ]
    model = q_ref.shape[1]
    q_ref[:LANES] = first_ref[...].reshape(model, LANES).T
    q_ref[LANES:] = rest_ref[...].reshape(model, LANES).T[:64]


def weights(place, mine, other, rows, q_width, kv_width):
    count = len(mine)
    blocks = (count, count, 2, rows)
    model = count * count * 2 * rows
    q_turned, kv = run(
        weights_kernel,
        [SMEM] + [VMEM] * (2 * count),
        (place, *mine, *other),
        [near((q_width, model), BF16), near((*blocks, kv_width), BF16)],
        [pltpu.VMEM((*blocks, LANES), BF16), pltpu.VMEM((*blocks, LANES), BF16)],
    )
    return q_turned, kv.reshape(model, kv_width)


NT = (((1,), (1,)), ((), ()))


def steps_kernel(place_ref, dir_ref, mine_ref, other_ref, own_ref, q_ref, kv_ref, own_out, factor_ref):
    q_width = q_ref.shape[0]
    factor = assemble(place_ref, mine_ref, other_ref, factor_ref)
    directions = dir_ref[...]
    turned = directions[:, :q_width].T
    q_ref[...] = lax.dot_general(turned, factor, NT, preferred_element_type=F32)
    kv_ref[...] = jnp.dot(factor, directions[:, q_width:], preferred_element_type=F32)
    own_out[...] = jnp.dot(own_ref[...], directions, preferred_element_type=F32)


def unscaled_steps(place, directions, mine, other, own, q_width):
    count, rows, rank = mine.shape
    model, width = 2 * count * rows, directions.shape[1]
    return run(
        steps_kernel,
        [SMEM] + [VMEM] * 4,
        (place, directions, mine, other, own),
        [near((q_width, model)), near((model, width - q_width)), near((own.shape[0], width))],
        [whole_factor(mine)],
        2 * width * rank * model,
    )


def finish_kernel(q_count, kv_count):
    def kernel(
        sums_ref, q_step_ref, kv_step_ref, own_ref, q_whole_ref, kv_whole_ref, q_ref, kv_ref,
        q_new, kv_new, q_step, kv_step, q_copy, kv_copy,
    ):
        q_width = q_ref.shape[1]
        sums = sums_ref[...]
        q_scale = 0.5 * jnp.sqrt(F32(q_count)) * lax.rsqrt(sums[0:1, 0:1] + 1e-06)
        kv_scale = 0.5 * jnp.sqrt(F32(kv_count)) * lax.rsqrt(sums[1:2, 0:1] + 1e-06)
        own = own_ref[...]
        step = q_scale * own[:, :q_width]
        q_step[...] = step
        q_new[...] = q_ref[...] - step
        step = kv_scale * own[:, q_width:]
        kv_step[...] = step
        kv_new[...] = kv_ref[...] - step
        q_copy[...] = (q_whole_ref[...].astype(F32) - q_scale * q_step_ref[...]).astype(BF16)
        kv_copy[...] = (kv_whole_ref[...].astype(F32) - kv_scale * kv_step_ref[...]).astype(BF16)

    return kernel


def finish(sums, q_steps, kv_steps, own, q_whole, kv_whole, q_own, kv_own, q_count, kv_count):
    return run(
        finish_kernel(q_count, kv_count),
        [VMEM] * 8,
        (sums, q_steps, kv_steps, own, q_whole, kv_whole, q_own, kv_own),
        [
            far(q_own.shape),
            far(kv_own.shape),
            far(q_own.shape),
            far(kv_own.shape),
            far(q_whole.shape, BF16),
            far(kv_whole.shape, BF16),
        ],
    )


def body(x, q_cot, kv_cot, row_factor, q_weight, kv_weight, qm, km, qs, ks):
    fs_count = lax.axis_size(FS)
    q_width, kv_width = q_cot.shape[1], kv_cot.shape[1]
    width, rank_rows = q_width + kv_width, qm.shape[0]
    place = jnp.stack([lax.axis_index(a) for a in ("z", "y", "core")]).astype(jnp.int32)
    factor_tiles, weight_rows = spread(row_factor, q_weight, kv_weight, lax.axis_size(ZY))
    mine = exchange(factor_tiles, ZY)
    grad = gradients(q_cot.T, kv_cot, x)
    other = swapped(mine, "core", 1)
    partial = project(place, mine, other, grad)
    parts = exchange(partial.reshape(fs_count, rank_rows, width), FS)
    weight_rows = stacked(shifted(weight_rows, "y"))
    to_send = direction_tiles(parts, (qm, km, qs, ks))
    qm_new, km_new, qs_new, ks_new = keep(parts, (qm, km, qs, ks))
    directions = exchange(to_send, FS).reshape(fs_count * rank_rows, width)
    weight_mine = shifted(weight_rows, "z")
    weight_other = [swapped(w, "core", 1) for w in weight_mine]
    q_whole, kv_whole = weights(
        place, weight_mine, weight_other, q_weight.shape[0], q_width, kv_width
    )
    squares = stats(directions, q_width)
    squares = squares + swapped(squares, "tp", 1)
    squares = squares + swapped(squares, "tp", 2)
    q_steps, kv_steps, own = unscaled_steps(
        place, directions, mine, other, row_factor, q_width
    )
    count = rank_rows * fs_count * lax.axis_size("tp")
    q_new, kv_new, q_step, kv_step, q_copy, kv_copy = finish(
        squares, q_steps, kv_steps, own, q_whole, kv_whole, q_weight, kv_weight,
        count * q_width, count * kv_width,
    )
    return (q_new, kv_new, q_step, kv_step, q_copy.T, kv_copy, qm_new, km_new, qs_new, ks_new)


def solution(mesh):
    split = Mesh(mesh.devices.reshape(4, 4, 2, mesh.shape["tp"]), ("z", "y", "core", "tp"))
    rows, tiles = P(FS, None), P(FS, "tp")
    return jax.shard_map(
        body,
        mesh=split,
        in_specs=(rows, tiles, tiles, rows, tiles, tiles, tiles, tiles, tiles, tiles),
        out_specs=(tiles, tiles, tiles, tiles, P(None, "tp"), P(None, "tp"), tiles, tiles, tiles, tiles),
        check_vma=False,
    )
```

```python
import jax
import jax.numpy as jnp
from jax import lax
from jax.experimental import pallas as pl
from jax.experimental.pallas import tpu as pltpu
from jax.sharding import Mesh
from jax.sharding import PartitionSpec as P


FS = ("z", "y", "core")
ZY = ("z", "y")
BF16 = jnp.bfloat16
F32 = jnp.float32
VMEM = pl.BlockSpec(memory_space=pltpu.MemorySpace.VMEM)
HBM = pl.BlockSpec(memory_space=pltpu.MemorySpace.HBM)
PLACES = {id(VMEM): pltpu.MemorySpace.VMEM, id(HBM): pltpu.MemorySpace.HBM}


def near(dims, kind=F32):
    return pltpu.MemorySpace.VMEM(dims, kind)


def far(dims, kind=F32):
    return jax.ShapeDtypeStruct(dims, kind)


def run(kernel, specs, operands, out, scratch=(), flops=0, limit=8, outs=None):
    operands = [
        pltpu.with_memory_space_constraint(o, PLACES[id(s)]) if id(s) in PLACES else o
        for s, o in zip(specs, operands)
    ]
    return pl.pallas_call(
        kernel,
        in_specs=list(specs),
        out_specs=outs or [VMEM] * len(out),
        out_shape=list(out),
        scratch_shapes=list(scratch),
        compiler_params=pltpu.CompilerParams(vmem_limit_bytes=limit * 1024 * 1024),
        cost_estimate=pl.CostEstimate(flops=flops, bytes_accessed=0, transcendentals=0),
    )(*operands)


def exchange(tiles, axis):
    return lax.all_to_all(tiles, axis, split_axis=0, concat_axis=0, tiled=True)


def swapped(array, axis, bit):
    count = lax.axis_size(axis)
    return lax.ppermute(array, axis, [(i, i ^ bit) for i in range(count)])


def shifted(array, axis, k):
    count = lax.axis_size(axis)
    return lax.ppermute(array, axis, [(i, (i + k) % count) for i in range(count)])


def fetch(pairs, sems):
    copies = [pltpu.make_async_copy(a, b, sems.at[i]) for i, (a, b) in enumerate(pairs)]
    for copy in copies:
        copy.start()
    for copy in copies:
        copy.wait()


LANES = 128
HALF = LANES // 2


def spread_kernel(
    factor_ref, q_ref, kv_ref, qm_ref, km_ref, qs_ref, ks_ref, factor_out, rows_out, moments_out,
    factor_buf, q_buf, kv_buf, qm_buf, km_buf, qs_buf, ks_buf, sems,
):
    fetch(
        (
            (factor_ref, factor_buf),
            (q_ref, q_buf),
            (kv_ref, kv_buf),
            (qm_ref, qm_buf),
            (km_ref, km_buf),
            (qs_ref, qs_buf),
            (ks_ref, ks_buf),
        ),
        sems,
    )
    factor = factor_buf[...]
    for i in range(factor_out.shape[0]):
        factor_out[i] = factor
    q_width = q_ref.shape[1]
    moments_out[0, :, :q_width] = qm_buf[...]
    moments_out[0, :, q_width:] = km_buf[...]
    moments_out[1, :, :q_width] = qs_buf[...]
    moments_out[1, :, q_width:] = ks_buf[...]
    rows = q_ref.shape[0]
    quarter = rows // 4
    q = q_buf[...].astype(BF16)
    rows_out[0, :rows, :LANES] = q[:, :LANES]
    rows_out[0, :rows, LANES:] = kv_buf[...].astype(BF16)
    for g in range(4):
        rows_out[0, rows:, HALF * g : HALF * (g + 1)] = q[quarter * g : quarter * (g + 1), LANES:]


def spread(factor, q, kv, qm, km, qs, ks, count):
    rows, width = q.shape[0], q.shape[1] + kv.shape[1]
    operands = (factor, q, kv, qm, km, qs, ks)
    return run(
        spread_kernel,
        [HBM] * 7,
        operands,
        [
            near((count, *factor.shape), BF16),
            near((1, rows + rows // 4, 2 * LANES), BF16),
            near((2, qm.shape[0], width)),
        ],
        [pltpu.VMEM(o.shape, o.dtype) for o in operands] + [pltpu.SemaphoreType.DMA((7,))],
    )


def stack_kernel(*refs):
    at = 0
    for ref in refs[:-1]:
        count = ref.shape[0]
        refs[-1][at : at + count] = ref[...]
        at += count


def stacked(tiles):
    count = sum(t.shape[0] for t in tiles)
    return run(
        stack_kernel, [VMEM] * len(tiles), tiles, [near((count, *tiles[0].shape[1:]), BF16)]
    )[0]


def gradient_kernel(q_ref, kv_ref, x_ref, out_ref, sum_ref, q_buf, kv_buf, x_buf, sems):
    depth, block, _ = x_buf.shape
    steps = x_ref.shape[0] // block

    def copies(k):
        at, slot = pl.ds(k * block, block), k % depth
        return (
            pltpu.make_async_copy(q_ref.at[:, at], q_buf.at[slot], sems.at[slot, 0]),
            pltpu.make_async_copy(kv_ref.at[at, :], kv_buf.at[slot], sems.at[slot, 1]),
            pltpu.make_async_copy(x_ref.at[at, :], x_buf.at[slot], sems.at[slot, 2]),
        )

    for k in range(depth):
        for copy in copies(k):
            copy.start()
    for k in range(steps):
        slot = k % depth
        for copy in copies(k):
            copy.wait()
        left = jnp.concatenate([q_buf[slot], kv_buf[slot].T], axis=0)
        piece = jnp.dot(left, x_buf[slot], preferred_element_type=F32)
        if k == 0:
            sum_ref[...] = piece
        elif k < steps - 1:
            sum_ref[...] += piece
        else:
            out_ref[...] = (sum_ref[...] + piece).astype(BF16)
        if k + depth < steps:
            for copy in copies(k + depth):
                copy.start()


def gradients(q_turned, kv, x, block=512, depth=4):
    q_width, kv_width = q_turned.shape[0], kv.shape[1]
    width = q_width + kv_width
    tokens, model = x.shape
    return run(
        gradient_kernel,
        [HBM] * 3,
        (q_turned, kv, x),
        [near((width, model), BF16)],
        [
            pltpu.VMEM((width, model), F32),
            pltpu.VMEM((depth, q_width, block), BF16),
            pltpu.VMEM((depth, block, kv_width), BF16),
            pltpu.VMEM((depth, block, model), BF16),
            pltpu.SemaphoreType.DMA((depth, 3)),
        ],
        2 * width * tokens * model,
        24,
    )[0]


def project_kernel(mine_ref, other_ref, grad_ref, out_ref, factor_ref):
    core = lax.axis_index("core")
    count, pair, rows, rank = factor_ref.shape
    for i in range(count):
        factor_ref[i, core] = mine_ref[i]
        factor_ref[i, 1 - core] = other_ref[i]
    factor = factor_ref[...].reshape(count * pair * rows, rank)
    out_ref[...] = jnp.dot(grad_ref[...], factor, preferred_element_type=F32).T.astype(BF16)


def project(mine, other, grad):
    count, rows, rank = mine.shape
    partial, factor = run(
        project_kernel,
        [VMEM] * 3,
        (mine, other, grad),
        [near((rank, grad.shape[0]), BF16), near((count, 2, rows, rank), BF16)],
    )
    return partial, factor.reshape(count * 2 * rows, rank)


def pair_kernel(parts_ref, moments_ref, out_ref):
    rows = parts_ref.shape[1]
    half = rows // 2
    out_ref[:rows] = jnp.sum(parts_ref[...].astype(F32), axis=0)
    out_ref[rows : rows + half] = moments_ref[0]
    out_ref[rows + half :] = moments_ref[1]


def pair_sums(parts, moments):
    rows, width = parts.shape[1:]
    return run(pair_kernel, [VMEM] * 2, (parts, moments), [near((2 * rows, width))])[0]


def update(value, first, second):
    return 0.8 * first + 0.2 * value, 0.9 * second + 0.1 * value * value


def direction_kernel(mine_ref, other_ref, out_ref, moments_ref):
    core = lax.axis_index("core")
    count, rows, _ = out_ref.shape
    half = rows // 2
    for ref, at in ((mine_ref, core * half), (other_ref, (1 - core) * half)):
        at = pl.ds(pl.multiple_of(at, half), half)
        moments_ref[0, at, :] = ref[rows : rows + half]
        moments_ref[1, at, :] = ref[rows + half :]
    value = mine_ref[:rows] + other_ref[:rows]
    first, second = update(value, moments_ref[0], moments_ref[1])
    direction = (first / (jnp.sqrt(second) + 1e-08)).astype(BF16)
    for i in range(count):
        out_ref[i] = direction


def direction_tiles(mine, other, count):
    rows, width = mine.shape[0] // 2, mine.shape[1]
    return run(
        direction_kernel,
        [VMEM] * 2,
        (mine, other),
        [near((count, rows, width), BF16)],
        [pltpu.VMEM((2, rows, width), F32)],
    )[0]


def keep_kernel(mine_ref, other_ref, qm_out, km_out, qs_out, ks_out):
    half, q_width = qm_out.shape
    rows = 2 * half
    at = pl.ds(pl.multiple_of(lax.axis_index("core") * half, half), half)
    value = mine_ref[at, :] + other_ref[at, :]
    first, second = update(value, mine_ref[rows : rows + half], mine_ref[rows + half :])
    qm_out[...] = first[:, :q_width]
    km_out[...] = first[:, q_width:]
    qs_out[...] = second[:, :q_width]
    ks_out[...] = second[:, q_width:]


def keep(mine, other, outs):
    return run(keep_kernel, [VMEM] * 2, (mine, other), [far(o.shape) for o in outs])


def stats_kernel(q_width):
    def kernel(dir_ref, out_ref):
        values = dir_ref[...].astype(F32)
        squares = jnp.sum(values * values, axis=0, keepdims=True)
        out_ref[0:1, :] = jnp.broadcast_to(jnp.sum(squares[:, :q_width], axis=1, keepdims=True), (1, 128))
        out_ref[1:2, :] = jnp.broadcast_to(jnp.sum(squares[:, q_width:], axis=1, keepdims=True), (1, 128))
        out_ref[2:, :] = jnp.zeros((6, 128), F32)

    return kernel


def stats(directions, q_width):
    return run(stats_kernel(q_width), [VMEM], (directions,), [near((8, 128))])[0]


def weights_kernel(*refs):
    tiles, (q_ref, kv_ref, first_ref, rest_ref) = refs[:-4], refs[-4:]
    z, y, core = (lax.axis_index(a) for a in ("z", "y", "core"))
    count = first_ref.shape[0]
    rows = first_ref.shape[3]
    quarter = rows // 4
    pieces = len(tiles) // 2
    half = count // 2
    origins = ((0, 0), (count - 1, 0), (1, 0), (half, 0), (half, half))
    for t, tile in enumerate(tiles):
        c = core if t < pieces else 1 - core
        dz, dy = origins[t % pieces]
        zi = lax.rem(z + dz, count)
        for k in range(tile.shape[0]):
            yi = lax.rem(y + count - dy - k, count)
            first_ref[zi, yi, c] = tile[k, :rows, :LANES]
            kv_ref[zi, yi, c] = tile[k, :rows, LANES:]
            for g in range(4):
                rest_ref[zi, yi, c, quarter * g : quarter * (g + 1), :HALF] = tile[
                    k, rows:, HALF * g : HALF * (g + 1)
                ]
    model = q_ref.shape[1]
    q_ref[:LANES] = first_ref[...].reshape(model, LANES).T
    q_ref[LANES:] = rest_ref[...].reshape(model, LANES).T[:HALF]


def weights(mine, other, rows, q_width, kv_width):
    count = mine[0].shape[0]
    blocks = (count, count, 2, rows)
    model = count * count * 2 * rows
    q_turned, kv = run(
        weights_kernel,
        [VMEM] * (2 * len(mine)),
        (*mine, *other),
        [near((q_width, model), BF16), near((*blocks, kv_width), BF16)],
        [pltpu.VMEM((*blocks, LANES), BF16), pltpu.VMEM((*blocks, LANES), BF16)],
    )
    return q_turned, kv.reshape(model, kv_width)


NT = (((1,), (1,)), ((), ()))


def steps_kernel(dir_ref, factor_ref, own_ref, q_ref, kv_ref, own_out):
    q_width = q_ref.shape[0]
    directions = dir_ref[...]
    factor = factor_ref[...]
    turned = directions[:, :q_width].T
    q_ref[...] = lax.dot_general(turned, factor, NT, preferred_element_type=F32)
    kv_ref[...] = jnp.dot(factor, directions[:, q_width:], preferred_element_type=F32)
    own_out[...] = jnp.dot(own_ref[...], directions, preferred_element_type=F32)


def unscaled_steps(directions, factor, own, q_width):
    model, width = factor.shape[0], directions.shape[1]
    return run(
        steps_kernel,
        [VMEM] * 3,
        (directions, factor, own),
        [near((q_width, model)), near((model, width - q_width)), near((own.shape[0], width))],
        flops=2 * width * directions.shape[0] * model,
    )


def finish_kernel(q_count, kv_count):
    def kernel(
        squares_0, squares_1, squares_2, squares_3, q_step_ref, kv_step_ref, own_ref, q_whole_ref, kv_whole_ref, q_ref, kv_ref,
        q_new, kv_new, q_step, kv_step, q_copy, kv_copy,
    ):
        q_width = q_ref.shape[1]
        sums = squares_0[...] + squares_1[...] + squares_2[...] + squares_3[...]
        q_scale = 0.5 * jnp.sqrt(F32(q_count)) * lax.rsqrt(sums[0:1, 0:1] + 1e-06)
        kv_scale = 0.5 * jnp.sqrt(F32(kv_count)) * lax.rsqrt(sums[1:2, 0:1] + 1e-06)
        own = own_ref[...]
        step = q_scale * own[:, :q_width]
        q_step[...] = step
        q_new[...] = q_ref[...] - step
        step = kv_scale * own[:, q_width:]
        kv_step[...] = step
        kv_new[...] = kv_ref[...] - step
        q_copy[...] = (q_whole_ref[...].astype(F32) - q_scale * q_step_ref[...]).astype(BF16)
        kv_copy[...] = (kv_whole_ref[...].astype(F32) - kv_scale * kv_step_ref[...]).astype(BF16)

    return kernel


def finish(squares, q_steps, kv_steps, own, q_whole, kv_whole, q_own, kv_own, q_count, kv_count):
    return run(
        finish_kernel(q_count, kv_count),
        [VMEM] * 11,
        (*squares, q_steps, kv_steps, own, q_whole, kv_whole, q_own, kv_own),
        [
            far(q_own.shape),
            far(kv_own.shape),
            far(q_own.shape),
            far(kv_own.shape),
            far(q_whole.shape, BF16),
            far(kv_whole.shape, BF16),
        ],
    )


def body(x, q_cot, kv_cot, row_factor, q_weight, kv_weight, qm, km, qs, ks):
    fs_count = lax.axis_size(FS)
    q_width, kv_width = q_cot.shape[1], kv_cot.shape[1]
    width, rank_rows = q_width + kv_width, qm.shape[0]
    chips = lax.axis_size(ZY)
    factor_tiles, weight_rows, moments = spread(
        row_factor, q_weight, kv_weight, qm, km, qs, ks, chips
    )
    mine = exchange(factor_tiles, ZY)
    grad = gradients(q_cot.T, kv_cot, x)
    mine, weight_rows, moments, grad = lax.optimization_barrier((mine, weight_rows, moments, grad))
    other = swapped(mine, "core", 1)
    weight_near = [shifted(weight_rows, "y", k) for k in (1, 2, 3)]
    partial, factor = project(mine, other, grad)
    parts = exchange(partial.reshape(chips, 2 * rank_rows, width), ZY)
    weight_stack = stacked((weight_rows, *weight_near))
    sums = pair_sums(parts, moments)
    more = swapped(sums, "core", 1)
    to_send = direction_tiles(sums, more, chips)
    qm_new, km_new, qs_new, ks_new = keep(sums, more, (qm, km, qs, ks))
    directions = exchange(to_send, ZY).reshape(fs_count * rank_rows, width)
    below = shifted(weight_stack, "z", 1)
    above = shifted(weight_stack, "z", 3)
    middle = weight_stack.shape[0] // 2
    weight_mine = (
        weight_stack, below, above, shifted(below[:middle], "z", 1), shifted(above[middle:], "z", 3)
    )
    weight_other = [swapped(w, "core", 1) for w in weight_mine]
    q_whole, kv_whole = weights(
        weight_mine, weight_other, q_weight.shape[0], q_width, kv_width
    )
    squares = stats(directions, q_width)
    squares = [squares] + [shifted(squares, "tp", k) for k in (2, 1, 3)]
    q_steps, kv_steps, own = unscaled_steps(directions, factor, row_factor, q_width)
    count = rank_rows * fs_count * lax.axis_size("tp")
    q_new, kv_new, q_step, kv_step, q_copy, kv_copy = finish(
        squares, q_steps, kv_steps, own, q_whole, kv_whole, q_weight, kv_weight,
        count * q_width, count * kv_width,
    )
    return (q_new, kv_new, q_step, kv_step, q_copy.T, kv_copy, qm_new, km_new, qs_new, ks_new)


def solution(mesh):
    split = Mesh(mesh.devices.reshape(4, 4, 2, mesh.shape["tp"]), ("z", "y", "core", "tp"))
    rows, tiles = P(FS, None), P(FS, "tp")
    return jax.shard_map(
        body,
        mesh=split,
        in_specs=(rows, tiles, tiles, rows, tiles, tiles, tiles, tiles, tiles, tiles),
        out_specs=(tiles, tiles, tiles, tiles, P(None, "tp"), P(None, "tp"), tiles, tiles, tiles, tiles),
        check_vma=False,
    )
```

```python
import jax
import jax.numpy as jnp
from jax import lax
from jax.experimental import pallas as pl
from jax.experimental.pallas import tpu as pltpu
from jax.sharding import Mesh
from jax.sharding import PartitionSpec as P


FS = ("z", "y", "core")
ZY = ("z", "y")
BF16 = jnp.bfloat16
F32 = jnp.float32
VMEM = pl.BlockSpec(memory_space=pltpu.MemorySpace.VMEM)
HBM = pl.BlockSpec(memory_space=pltpu.MemorySpace.HBM)
PLACES = {id(VMEM): pltpu.MemorySpace.VMEM, id(HBM): pltpu.MemorySpace.HBM}


def near(dims, kind=F32):
    return pltpu.MemorySpace.VMEM(dims, kind)


def far(dims, kind=F32):
    return jax.ShapeDtypeStruct(dims, kind)


def run(kernel, specs, operands, out, scratch=(), flops=0, limit=8, outs=None):
    operands = [
        pltpu.with_memory_space_constraint(o, PLACES[id(s)]) if id(s) in PLACES else o
        for s, o in zip(specs, operands)
    ]
    return pl.pallas_call(
        kernel,
        in_specs=list(specs),
        out_specs=outs or [VMEM] * len(out),
        out_shape=list(out),
        scratch_shapes=list(scratch),
        compiler_params=pltpu.CompilerParams(vmem_limit_bytes=limit * 1024 * 1024),
        cost_estimate=pl.CostEstimate(flops=flops, bytes_accessed=0, transcendentals=0),
    )(*operands)


def exchange(tiles, axis):
    return lax.all_to_all(tiles, axis, split_axis=0, concat_axis=0, tiled=True)


def swapped(array, axis, bit):
    count = lax.axis_size(axis)
    return lax.ppermute(array, axis, [(i, i ^ bit) for i in range(count)])


def shifted(array, axis, k):
    count = lax.axis_size(axis)
    return lax.ppermute(array, axis, [(i, (i + k) % count) for i in range(count)])


def turned(array, axis):
    sizes = [lax.axis_size(a) for a in FS]
    at = FS.index(axis)
    pairs = []
    for z in range(sizes[0]):
        for y in range(sizes[1]):
            for core in range(sizes[2]):
                here, there = [z, y, core], [z, y, core]
                there[at] = (there[at] + 2 * core - 1) % sizes[at]
                pairs.append(
                    tuple((p[0] * sizes[1] + p[1]) * sizes[2] + p[2] for p in (here, there))
                )
    return lax.ppermute(array, FS, pairs)


LANES = 128
HALF = LANES // 2


def spread_kernel(factor_ref, out_ref, buf_ref, sems):
    count = out_ref.shape[0]
    arrival = pltpu.make_async_copy(factor_ref, buf_ref, sems.at[count])
    arrival.start()
    arrival.wait()
    copies = [pltpu.make_async_copy(buf_ref, out_ref.at[i], sems.at[i]) for i in range(count)]
    for copy in copies:
        copy.start()
    for copy in copies:
        copy.wait()


def spread(factor, count):
    return run(
        spread_kernel,
        [HBM],
        (factor,),
        [far((count, *factor.shape), BF16)],
        [pltpu.VMEM(factor.shape, BF16), pltpu.SemaphoreType.DMA((count + 1,))],
        outs=[HBM],
    )[0]


def fold(q_ref, kv_ref, out_ref):
    rows = q_ref.shape[0]
    quarter = rows // 4
    q = q_ref[...].astype(BF16)
    out_ref[0, :rows, :LANES] = q[:, :LANES]
    out_ref[0, :rows, LANES:] = kv_ref[...].astype(BF16)
    for g in range(4):
        out_ref[0, rows:, HALF * g : HALF * (g + 1)] = q[quarter * g : quarter * (g + 1), LANES:]


def stack_kernel(*refs):
    at = 0
    for ref in refs[:-1]:
        count = ref.shape[0]
        refs[-1][at : at + count] = ref[...]
        at += count


def stacked(tiles):
    count = sum(t.shape[0] for t in tiles)
    return run(
        stack_kernel, [VMEM] * len(tiles), tiles, [near((count, *tiles[0].shape[1:]), BF16)]
    )[0]


def gradient_kernel(
    q_ref, kv_ref, x_ref, qw_ref, kvw_ref, qm_ref, km_ref, qs_ref, ks_ref,
    out_ref, rows_ref, moments_ref, sum_ref, q_buf, kv_buf, x_buf,
    qw_buf, kvw_buf, qm_buf, km_buf, qs_buf, ks_buf, sems, small_sems,
):
    depth, block, _ = x_buf.shape
    steps = x_ref.shape[0] // block
    q_width = q_ref.shape[0]

    def copies(k):
        at, slot = pl.ds(k * block, block), k % depth
        return (
            pltpu.make_async_copy(q_ref.at[:, at], q_buf.at[slot], sems.at[slot, 0]),
            pltpu.make_async_copy(kv_ref.at[at, :], kv_buf.at[slot], sems.at[slot, 1]),
            pltpu.make_async_copy(x_ref.at[at, :], x_buf.at[slot], sems.at[slot, 2]),
        )

    small = [
        pltpu.make_async_copy(a, b, small_sems.at[i])
        for i, (a, b) in enumerate(
            (
                (qw_ref, qw_buf),
                (kvw_ref, kvw_buf),
                (qm_ref, qm_buf),
                (km_ref, km_buf),
                (qs_ref, qs_buf),
                (ks_ref, ks_buf),
            )
        )
    ]
    for k in range(depth):
        for copy in copies(k):
            copy.start()
    for copy in small:
        copy.start()
    for k in range(steps):
        slot = k % depth
        for copy in copies(k):
            copy.wait()
        left = jnp.concatenate([q_buf[slot], kv_buf[slot].T], axis=0)
        piece = jnp.dot(left, x_buf[slot], preferred_element_type=F32)
        if k == 0:
            sum_ref[...] = piece
        elif k < steps - 1:
            sum_ref[...] += piece
        else:
            out_ref[...] = (sum_ref[...] + piece).astype(BF16)
        if k + depth < steps:
            for copy in copies(k + depth):
                copy.start()
        if k == depth:
            for copy in small:
                copy.wait()
            fold(qw_buf, kvw_buf, rows_ref)
            moments_ref[0, :, :q_width] = qm_buf[...]
            moments_ref[0, :, q_width:] = km_buf[...]
            moments_ref[1, :, :q_width] = qs_buf[...]
            moments_ref[1, :, q_width:] = ks_buf[...]


def gradients(q_turned, kv, x, small, block=512, depth=4):
    q_width, kv_width = q_turned.shape[0], kv.shape[1]
    width = q_width + kv_width
    tokens, model = x.shape
    rows, half = small[0].shape[0], small[2].shape[0]
    return run(
        gradient_kernel,
        [HBM] * (3 + len(small)),
        (q_turned, kv, x, *small),
        [
            near((width, model), BF16),
            near((1, rows + rows // 4, 2 * LANES), BF16),
            near((2, half, width)),
        ],
        [
            pltpu.VMEM((width, model), F32),
            pltpu.VMEM((depth, q_width, block), BF16),
            pltpu.VMEM((depth, block, kv_width), BF16),
            pltpu.VMEM((depth, block, model), BF16),
        ]
        + [pltpu.VMEM(a.shape, F32) for a in small]
        + [pltpu.SemaphoreType.DMA((depth, 3)), pltpu.SemaphoreType.DMA((len(small),))],
        2 * width * tokens * model,
        24,
    )


def project_kernel(mine_ref, other_ref, grad_ref, out_ref, factor_ref):
    core = lax.axis_index("core")
    count, pair, rows, rank = factor_ref.shape
    for i in range(count):
        factor_ref[i, core] = mine_ref[i]
        factor_ref[i, 1 - core] = other_ref[i]
    factor = factor_ref[...].reshape(count * pair * rows, rank)
    out_ref[...] = jnp.dot(grad_ref[...], factor, preferred_element_type=F32).T.astype(BF16)


def project(mine, other, grad):
    count, rows, rank = mine.shape
    partial, factor = run(
        project_kernel,
        [VMEM] * 3,
        (mine, other, grad),
        [near((rank, grad.shape[0]), BF16), near((count, 2, rows, rank), BF16)],
    )
    return partial, factor.reshape(count * 2 * rows, rank)


def pair_kernel(parts_ref, moments_ref, out_ref):
    rows = parts_ref.shape[1]
    half = rows // 2
    out_ref[:rows] = jnp.sum(parts_ref[...].astype(F32), axis=0)
    out_ref[rows : rows + half] = moments_ref[0]
    out_ref[rows + half :] = moments_ref[1]


def pair_sums(parts, moments):
    rows, width = parts.shape[1:]
    return run(pair_kernel, [VMEM] * 2, (parts, moments), [near((2 * rows, width))])[0]


def update(value, first, second):
    return 0.8 * first + 0.2 * value, 0.9 * second + 0.1 * value * value


def direction_kernel(mine_ref, other_ref, out_ref, moments_ref):
    core = lax.axis_index("core")
    count, rows, _ = out_ref.shape
    half = rows // 2
    for ref, at in ((mine_ref, core * half), (other_ref, (1 - core) * half)):
        at = pl.ds(pl.multiple_of(at, half), half)
        moments_ref[0, at, :] = ref[rows : rows + half]
        moments_ref[1, at, :] = ref[rows + half :]
    value = mine_ref[:rows] + other_ref[:rows]
    first, second = update(value, moments_ref[0], moments_ref[1])
    direction = (first / (jnp.sqrt(second) + 1e-08)).astype(BF16)
    for i in range(count):
        out_ref[i] = direction


def direction_tiles(mine, other, count):
    rows, width = mine.shape[0] // 2, mine.shape[1]
    return run(
        direction_kernel,
        [VMEM] * 2,
        (mine, other),
        [near((count, rows, width), BF16)],
        [pltpu.VMEM((2, rows, width), F32)],
    )[0]


def stats_kernel(q_width):
    def kernel(dir_ref, out_ref):
        values = dir_ref[...].astype(F32)
        squares = jnp.sum(values * values, axis=0, keepdims=True)
        out_ref[0:1, :] = jnp.broadcast_to(jnp.sum(squares[:, :q_width], axis=1, keepdims=True), (1, 128))
        out_ref[1:2, :] = jnp.broadcast_to(jnp.sum(squares[:, q_width:], axis=1, keepdims=True), (1, 128))
        out_ref[2:, :] = jnp.zeros((6, 128), F32)

    return kernel


def stats(directions, q_width):
    return run(stats_kernel(q_width), [VMEM], (directions,), [near((8, 128))])[0]


def weights_kernel(here_ref, near_ref, over_ref, far_ref, last_ref, q_ref, kv_ref, first_ref, rest_ref):
    z, y, core = (lax.axis_index(a) for a in FS)
    count, _, _, rows, _ = first_ref.shape
    quarter = rows // 4
    turn = 2 * core - 1

    def around(value):
        return lax.rem(value + count, count)

    def pieces(c):
        t = 2 * c - 1
        return [(y, c), (around(y - t), c), (around(y - t), 1 - c), (around(y + count // 2), c)]

    mine, other = pieces(core), pieces(1 - core)
    for ref, zi, order in (
        (here_ref, z, mine + other),
        (near_ref, around(z - turn), mine + other),
        (over_ref, around(z + turn), other + mine),
        (far_ref, around(z + count // 2), mine),
        (last_ref, around(z + count // 2), other),
    ):
        for k, (yi, c) in enumerate(order):
            first_ref[zi, yi, c] = ref[k, :rows, :LANES]
            kv_ref[zi, yi, c] = ref[k, :rows, LANES:]
            for g in range(4):
                rest_ref[zi, yi, c, quarter * g : quarter * (g + 1), :HALF] = ref[
                    k, rows:, HALF * g : HALF * (g + 1)
                ]
    model = q_ref.shape[1]
    q_ref[:LANES] = first_ref[...].reshape(model, LANES).T
    q_ref[LANES:] = rest_ref[...].reshape(model, LANES).T[:HALF]


def weights(pieces, count, rows, q_width, kv_width):
    blocks = (count, count, 2, rows)
    model = count * count * 2 * rows
    q_turned, kv = run(
        weights_kernel,
        [VMEM] * len(pieces),
        pieces,
        [near((q_width, model), BF16), near((*blocks, kv_width), BF16)],
        [pltpu.VMEM((*blocks, LANES), BF16), pltpu.VMEM((*blocks, LANES), BF16)],
    )
    return q_turned, kv.reshape(model, kv_width)


NT = (((1,), (1,)), ((), ()))


def steps_kernel(
    dir_ref, factor_ref, own_ref, mine_ref, other_ref,
    q_ref, kv_ref, own_out, qm_out, km_out, qs_out, ks_out, qm_buf, km_buf, qs_buf, ks_buf, sems,
):
    half, q_width = qm_buf.shape
    rows = 2 * half
    at = pl.ds(pl.multiple_of(lax.axis_index("core") * half, half), half)
    value = mine_ref[at, :] + other_ref[at, :]
    first, second = update(value, mine_ref[rows : rows + half], mine_ref[rows + half :])
    qm_buf[...] = first[:, :q_width]
    km_buf[...] = first[:, q_width:]
    qs_buf[...] = second[:, :q_width]
    ks_buf[...] = second[:, q_width:]
    saved = [
        pltpu.make_async_copy(a, b, sems.at[i])
        for i, (a, b) in enumerate(
            ((qm_buf, qm_out), (km_buf, km_out), (qs_buf, qs_out), (ks_buf, ks_out))
        )
    ]
    for copy in saved:
        copy.start()
    directions = dir_ref[...]
    factor = factor_ref[...]
    turned = directions[:, :q_width].T
    q_ref[...] = lax.dot_general(turned, factor, NT, preferred_element_type=F32)
    kv_ref[...] = jnp.dot(factor, directions[:, q_width:], preferred_element_type=F32)
    own_out[...] = jnp.dot(own_ref[...], directions, preferred_element_type=F32)
    for copy in saved:
        copy.wait()


def unscaled_steps(directions, factor, own, mine, other, kept):
    model, width = factor.shape[0], directions.shape[1]
    q_width = kept[0].shape[1]
    return run(
        steps_kernel,
        [VMEM] * 5,
        (directions, factor, own, mine, other),
        [near((q_width, model)), near((model, width - q_width)), near((own.shape[0], width))]
        + [far(k.shape) for k in kept],
        [pltpu.VMEM(k.shape, F32) for k in kept] + [pltpu.SemaphoreType.DMA((len(kept),))],
        2 * width * directions.shape[0] * model,
        outs=[VMEM] * 3 + [HBM] * 4,
    )


PARTS = 2


def finish_kernel(q_count, kv_count):
    def kernel(
        squares_0, squares_1, squares_2, squares_3, q_step_ref, kv_step_ref, own_ref, q_whole_ref,
        kv_whole_ref, q_ref, kv_ref, q_new, kv_new, q_step, kv_step, q_copy, kv_copy,
        q_new_buf, kv_new_buf, q_step_buf, kv_step_buf, q_buf, kv_buf, sems,
    ):
        copies = []

        def save(source, target):
            copy = pltpu.make_async_copy(source, target, sems.at[len(copies)])
            copy.start()
            copies.append(copy)

        q_width, model = q_buf.shape
        piece = model // PARTS
        sums = squares_0[...] + squares_1[...] + squares_2[...] + squares_3[...]
        q_scale = 0.5 * jnp.sqrt(F32(q_count)) * lax.rsqrt(sums[0:1, 0:1] + 1e-06)
        kv_scale = 0.5 * jnp.sqrt(F32(kv_count)) * lax.rsqrt(sums[1:2, 0:1] + 1e-06)
        own = own_ref[...]
        step = q_scale * own[:, :q_width]
        q_step_buf[...] = step
        q_new_buf[...] = q_ref[...] - step
        step = kv_scale * own[:, q_width:]
        kv_step_buf[...] = step
        kv_new_buf[...] = kv_ref[...] - step
        save(q_step_buf, q_step)
        save(q_new_buf, q_new)
        save(kv_step_buf, kv_step)
        save(kv_new_buf, kv_new)
        for p in range(PARTS):
            at = slice(p * piece, (p + 1) * piece)
            q_buf[:, at] = (q_whole_ref[:, at].astype(F32) - q_scale * q_step_ref[:, at]).astype(BF16)
            save(q_buf.at[:, at], q_copy.at[:, at])
        for p in range(PARTS):
            at = slice(p * piece, (p + 1) * piece)
            kv_buf[at] = (kv_whole_ref[at].astype(F32) - kv_scale * kv_step_ref[at]).astype(BF16)
            save(kv_buf.at[at], kv_copy.at[at])
        for copy in copies:
            copy.wait()

    return kernel


def finish(squares, q_steps, kv_steps, own, q_whole, kv_whole, q_own, kv_own, q_count, kv_count):
    made = [
        (q_own.shape, F32),
        (kv_own.shape, F32),
        (q_own.shape, F32),
        (kv_own.shape, F32),
        (q_whole.shape, BF16),
        (kv_whole.shape, BF16),
    ]
    return run(
        finish_kernel(q_count, kv_count),
        [VMEM] * 11,
        (*squares, q_steps, kv_steps, own, q_whole, kv_whole, q_own, kv_own),
        [far(*m) for m in made],
        [pltpu.VMEM(*m) for m in made] + [pltpu.SemaphoreType.DMA((4 + 2 * PARTS,))],
        outs=[HBM] * 6,
    )


def body(x, q_cot, kv_cot, row_factor, q_weight, kv_weight, qm, km, qs, ks):
    fs_count = lax.axis_size(FS)
    q_width, kv_width = q_cot.shape[1], kv_cot.shape[1]
    width, rank_rows = q_width + kv_width, qm.shape[0]
    chips = lax.axis_size(ZY)
    mine = exchange(spread(row_factor, chips), ZY)
    grad, weight_rows, moments = gradients(
        q_cot.T, kv_cot, x, (q_weight, kv_weight, qm, km, qs, ks)
    )
    mine, grad, weight_rows, moments = lax.optimization_barrier((mine, grad, weight_rows, moments))
    weight_more = swapped(weight_rows, "core", 1)
    other = swapped(mine, "core", 1)
    weight_across = shifted(weight_rows, "y", lax.axis_size("y") // 2)
    weight_both = stacked((weight_rows, weight_more))
    weight_beside = turned(weight_both, "y")
    partial, factor = project(mine, other, grad)
    parts = exchange(partial.reshape(chips, 2 * rank_rows, width), ZY)
    weight_part = stacked((weight_rows, weight_beside, weight_across))
    weight_row = stacked((weight_part, swapped(weight_part, "core", 1)))
    weight_near = turned(weight_row, "z")
    sums = pair_sums(parts, moments)
    more = swapped(sums, "core", 1)
    to_send = direction_tiles(sums, more, chips)
    directions = exchange(to_send, ZY).reshape(fs_count * rank_rows, width)
    weight_over = swapped(weight_near, "core", 1)
    weight_far = shifted(weight_part, "z", lax.axis_size("z") // 2)
    weight_last = swapped(weight_far, "core", 1)
    q_whole, kv_whole = weights(
        (weight_row, weight_near, weight_over, weight_far, weight_last),
        lax.axis_size("z"), q_weight.shape[0], q_width, kv_width,
    )
    squares = stats(directions, q_width)
    squares = [squares] + [shifted(squares, "tp", k) for k in (2, 1, 3)]
    q_steps, kv_steps, own, *kept = unscaled_steps(
        directions, factor, row_factor, sums, more, (qm, km, qs, ks)
    )
    count = rank_rows * fs_count * lax.axis_size("tp")
    q_new, kv_new, q_step, kv_step, q_copy, kv_copy = finish(
        squares, q_steps, kv_steps, own, q_whole, kv_whole, q_weight, kv_weight,
        count * q_width, count * kv_width,
    )
    return (q_new, kv_new, q_step, kv_step, q_copy.T, kv_copy, *kept)


def solution(mesh):
    split = Mesh(mesh.devices.reshape(4, 4, 2, mesh.shape["tp"]), ("z", "y", "core", "tp"))
    rows, tiles = P(FS, None), P(FS, "tp")
    return jax.shard_map(
        body,
        mesh=split,
        in_specs=(rows, tiles, tiles, rows, tiles, tiles, tiles, tiles, tiles, tiles),
        out_specs=(tiles, tiles, tiles, tiles, P(None, "tp"), P(None, "tp"), tiles, tiles, tiles, tiles),
        check_vma=False,
    )
```

```python
import jax
import jax.numpy as jnp
from jax import lax
from jax.experimental import pallas as pl
from jax.experimental.pallas import tpu as pltpu
from jax.sharding import Mesh
from jax.sharding import PartitionSpec as P


FS = ("z", "y", "core")
ZY = ("z", "y")
BF16 = jnp.bfloat16
F32 = jnp.float32
VMEM = pl.BlockSpec(memory_space=pltpu.MemorySpace.VMEM)
HBM = pl.BlockSpec(memory_space=pltpu.MemorySpace.HBM)
PLACES = {id(VMEM): pltpu.MemorySpace.VMEM, id(HBM): pltpu.MemorySpace.HBM}


def near(dims, kind=F32):
    return pltpu.MemorySpace.VMEM(dims, kind)


def far(dims, kind=F32):
    return jax.ShapeDtypeStruct(dims, kind)


def run(kernel, specs, operands, out, scratch=(), flops=0, limit=8, outs=None):
    operands = [
        pltpu.with_memory_space_constraint(o, PLACES[id(s)]) if id(s) in PLACES else o
        for s, o in zip(specs, operands)
    ]
    return pl.pallas_call(
        kernel,
        in_specs=list(specs),
        out_specs=outs or [VMEM] * len(out),
        out_shape=list(out),
        scratch_shapes=list(scratch),
        compiler_params=pltpu.CompilerParams(vmem_limit_bytes=limit * 1024 * 1024),
        cost_estimate=pl.CostEstimate(flops=flops, bytes_accessed=0, transcendentals=0),
    )(*operands)


def exchange(tiles, axis):
    return lax.all_to_all(tiles, axis, split_axis=0, concat_axis=0, tiled=True)


def swapped(array, axis, bit):
    count = lax.axis_size(axis)
    return lax.ppermute(array, axis, [(i, i ^ bit) for i in range(count)])


def shifted(array, axis, k):
    count = lax.axis_size(axis)
    return lax.ppermute(array, axis, [(i, (i + k) % count) for i in range(count)])


def turned(array, axis):
    sizes = [lax.axis_size(a) for a in FS]
    at = FS.index(axis)
    pairs = []
    for z in range(sizes[0]):
        for y in range(sizes[1]):
            for core in range(sizes[2]):
                here, there = [z, y, core], [z, y, core]
                there[at] = (there[at] + 2 * core - 1) % sizes[at]
                pairs.append(
                    tuple((p[0] * sizes[1] + p[1]) * sizes[2] + p[2] for p in (here, there))
                )
    return lax.ppermute(array, FS, pairs)


def fetch(pairs, sems):
    copies = [pltpu.make_async_copy(a, b, sems.at[i]) for i, (a, b) in enumerate(pairs)]
    for copy in copies:
        copy.start()
    for copy in copies:
        copy.wait()


LANES = 128
HALF = LANES // 2


def spread_kernel(
    factor_ref, q_ref, kv_ref, qm_ref, km_ref, qs_ref, ks_ref, factor_out, rows_out, moments_out,
    factor_buf, q_buf, kv_buf, qm_buf, km_buf, qs_buf, ks_buf, sems,
):
    fetch(
        (
            (factor_ref, factor_buf),
            (q_ref, q_buf),
            (kv_ref, kv_buf),
            (qm_ref, qm_buf),
            (km_ref, km_buf),
            (qs_ref, qs_buf),
            (ks_ref, ks_buf),
        ),
        sems,
    )
    factor = factor_buf[...]
    for i in range(factor_out.shape[0]):
        factor_out[i] = factor
    q_width = q_ref.shape[1]
    moments_out[0, :, :q_width] = qm_buf[...]
    moments_out[0, :, q_width:] = km_buf[...]
    moments_out[1, :, :q_width] = qs_buf[...]
    moments_out[1, :, q_width:] = ks_buf[...]
    rows = q_ref.shape[0]
    quarter = rows // 4
    q = q_buf[...].astype(BF16)
    rows_out[0, :rows, :LANES] = q[:, :LANES]
    rows_out[0, :rows, LANES:] = kv_buf[...].astype(BF16)
    for g in range(4):
        rows_out[0, rows:, HALF * g : HALF * (g + 1)] = q[quarter * g : quarter * (g + 1), LANES:]


def spread(factor, q, kv, qm, km, qs, ks, count):
    rows, width = q.shape[0], q.shape[1] + kv.shape[1]
    operands = (factor, q, kv, qm, km, qs, ks)
    return run(
        spread_kernel,
        [HBM] * 7,
        operands,
        [
            near((count, *factor.shape), BF16),
            near((1, rows + rows // 4, 2 * LANES), BF16),
            near((2, qm.shape[0], width)),
        ],
        [pltpu.VMEM(o.shape, o.dtype) for o in operands] + [pltpu.SemaphoreType.DMA((7,))],
    )


def stack_kernel(*refs):
    at = 0
    for ref in refs[:-1]:
        count = ref.shape[0]
        refs[-1][at : at + count] = ref[...]
        at += count


def stacked(tiles):
    count = sum(t.shape[0] for t in tiles)
    return run(
        stack_kernel, [VMEM] * len(tiles), tiles, [near((count, *tiles[0].shape[1:]), BF16)]
    )[0]


def gradient_kernel(
    q_ref, kv_ref, x_ref, rows_ref, more_ref, out_ref, both_ref, sum_ref, q_buf, kv_buf, x_buf, sems
):
    depth, block, _ = x_buf.shape
    steps = x_ref.shape[0] // block

    def copies(k):
        at, slot = pl.ds(k * block, block), k % depth
        return (
            pltpu.make_async_copy(q_ref.at[:, at], q_buf.at[slot], sems.at[slot, 0]),
            pltpu.make_async_copy(kv_ref.at[at, :], kv_buf.at[slot], sems.at[slot, 1]),
            pltpu.make_async_copy(x_ref.at[at, :], x_buf.at[slot], sems.at[slot, 2]),
        )

    for k in range(depth):
        for copy in copies(k):
            copy.start()
    both_ref[0] = rows_ref[0]
    both_ref[1] = more_ref[0]
    for k in range(steps):
        slot = k % depth
        for copy in copies(k):
            copy.wait()
        left = jnp.concatenate([q_buf[slot], kv_buf[slot].T], axis=0)
        piece = jnp.dot(left, x_buf[slot], preferred_element_type=F32)
        if k == 0:
            sum_ref[...] = piece
        elif k < steps - 1:
            sum_ref[...] += piece
        else:
            out_ref[...] = (sum_ref[...] + piece).astype(BF16)
        if k + depth < steps:
            for copy in copies(k + depth):
                copy.start()


def gradients(q_turned, kv, x, rows, more, block=512, depth=4):
    q_width, kv_width = q_turned.shape[0], kv.shape[1]
    width = q_width + kv_width
    tokens, model = x.shape
    return run(
        gradient_kernel,
        [HBM] * 3 + [VMEM] * 2,
        (q_turned, kv, x, rows, more),
        [near((width, model), BF16), near((2, *rows.shape[1:]), BF16)],
        [
            pltpu.VMEM((width, model), F32),
            pltpu.VMEM((depth, q_width, block), BF16),
            pltpu.VMEM((depth, block, kv_width), BF16),
            pltpu.VMEM((depth, block, model), BF16),
            pltpu.SemaphoreType.DMA((depth, 3)),
        ],
        2 * width * tokens * model,
        24,
    )


def project_kernel(mine_ref, other_ref, grad_ref, out_ref, factor_ref):
    core = lax.axis_index("core")
    count, pair, rows, rank = factor_ref.shape
    for i in range(count):
        factor_ref[i, core] = mine_ref[i]
        factor_ref[i, 1 - core] = other_ref[i]
    factor = factor_ref[...].reshape(count * pair * rows, rank)
    out_ref[...] = jnp.dot(grad_ref[...], factor, preferred_element_type=F32).T.astype(BF16)


def project(mine, other, grad):
    count, rows, rank = mine.shape
    partial, factor = run(
        project_kernel,
        [VMEM] * 3,
        (mine, other, grad),
        [near((rank, grad.shape[0]), BF16), near((count, 2, rows, rank), BF16)],
    )
    return partial, factor.reshape(count * 2 * rows, rank)


def update(value, first, second):
    return 0.8 * first + 0.2 * value, 0.9 * second + 0.1 * value * value


def direction_kernel(parts_ref, moments_ref, out_ref, sums_ref):
    value = jnp.sum(parts_ref[...].astype(F32), axis=0)
    sums_ref[...] = value
    first, second = update(value, moments_ref[0], moments_ref[1])
    direction = (first / (jnp.sqrt(second) + 1e-08)).astype(BF16)
    for i in range(out_ref.shape[0]):
        out_ref[i] = direction


def direction_tiles(parts, moments):
    return run(
        direction_kernel,
        [VMEM] * 2,
        (parts, moments),
        [near(parts.shape, BF16), near(parts.shape[1:])],
    )


def stats_kernel(q_width):
    def kernel(dir_ref, out_ref):
        values = dir_ref[...].astype(F32)
        squares = jnp.sum(values * values, axis=0, keepdims=True)
        out_ref[0:1, :] = jnp.broadcast_to(jnp.sum(squares[:, :q_width], axis=1, keepdims=True), (1, 128))
        out_ref[1:2, :] = jnp.broadcast_to(jnp.sum(squares[:, q_width:], axis=1, keepdims=True), (1, 128))
        out_ref[2:, :] = jnp.zeros((6, 128), F32)

    return kernel


def stats(directions, q_width):
    return run(stats_kernel(q_width), [VMEM], (directions,), [near((8, 128))])[0]


def weights_kernel(here_ref, near_ref, over_ref, far_ref, last_ref, q_ref, kv_ref, first_ref, rest_ref):
    z, y, core = (lax.axis_index(a) for a in FS)
    count, _, _, rows, _ = first_ref.shape
    quarter = rows // 4
    turn = 2 * core - 1

    def around(value):
        return lax.rem(value + count, count)

    def pieces(c):
        t = 2 * c - 1
        return [(y, c), (around(y - t), c), (around(y - t), 1 - c), (around(y + count // 2), c)]

    mine, other = pieces(core), pieces(1 - core)
    for ref, zi, order in (
        (here_ref, z, mine + other),
        (near_ref, around(z - turn), mine + other),
        (over_ref, around(z + turn), other + mine),
        (far_ref, around(z + count // 2), mine),
        (last_ref, around(z + count // 2), other),
    ):
        for k, (yi, c) in enumerate(order):
            first_ref[zi, yi, c] = ref[k, :rows, :LANES]
            kv_ref[zi, yi, c] = ref[k, :rows, LANES:]
            for g in range(4):
                rest_ref[zi, yi, c, quarter * g : quarter * (g + 1), :HALF] = ref[
                    k, rows:, HALF * g : HALF * (g + 1)
                ]
    model = q_ref.shape[1]
    q_ref[:LANES] = first_ref[...].reshape(model, LANES).T
    q_ref[LANES:] = rest_ref[...].reshape(model, LANES).T[:HALF]


def weights(pieces, count, rows, q_width, kv_width):
    blocks = (count, count, 2, rows)
    model = count * count * 2 * rows
    q_turned, kv = run(
        weights_kernel,
        [VMEM] * len(pieces),
        pieces,
        [near((q_width, model), BF16), near((*blocks, kv_width), BF16)],
        [pltpu.VMEM((*blocks, LANES), BF16), pltpu.VMEM((*blocks, LANES), BF16)],
    )
    return q_turned, kv.reshape(model, kv_width)


NT = (((1,), (1,)), ((), ()))


def steps_kernel(
    dir_ref, factor_ref, own_ref, sums_ref, moments_ref,
    q_ref, kv_ref, own_out, qm_out, km_out, qs_out, ks_out, qm_buf, km_buf, qs_buf, ks_buf, sems,
):
    q_width = qm_buf.shape[1]
    first, second = update(sums_ref[...], moments_ref[0], moments_ref[1])
    qm_buf[...] = first[:, :q_width]
    km_buf[...] = first[:, q_width:]
    qs_buf[...] = second[:, :q_width]
    ks_buf[...] = second[:, q_width:]
    saved = [
        pltpu.make_async_copy(a, b, sems.at[i])
        for i, (a, b) in enumerate(
            ((qm_buf, qm_out), (km_buf, km_out), (qs_buf, qs_out), (ks_buf, ks_out))
        )
    ]
    for copy in saved:
        copy.start()
    directions = dir_ref[...]
    factor = factor_ref[...]
    turned = directions[:, :q_width].T
    q_ref[...] = lax.dot_general(turned, factor, NT, preferred_element_type=F32)
    kv_ref[...] = jnp.dot(factor, directions[:, q_width:], preferred_element_type=F32)
    own_out[...] = jnp.dot(own_ref[...], directions, preferred_element_type=F32)
    for copy in saved:
        copy.wait()


def unscaled_steps(directions, factor, own, sums, moments, kept):
    model, width = factor.shape[0], directions.shape[1]
    q_width = kept[0].shape[1]
    return run(
        steps_kernel,
        [VMEM] * 5,
        (directions, factor, own, sums, moments),
        [near((q_width, model)), near((model, width - q_width)), near((own.shape[0], width))]
        + [far(k.shape) for k in kept],
        [pltpu.VMEM(k.shape, F32) for k in kept] + [pltpu.SemaphoreType.DMA((len(kept),))],
        2 * width * directions.shape[0] * model,
        outs=[VMEM] * 3 + [HBM] * 4,
    )


PARTS = 2


def finish_kernel(q_count, kv_count):
    def kernel(
        squares_0, squares_1, squares_2, squares_3, q_step_ref, kv_step_ref, own_ref, q_whole_ref,
        kv_whole_ref, q_ref, kv_ref, q_new, kv_new, q_step, kv_step, q_copy, kv_copy,
        q_new_buf, kv_new_buf, q_step_buf, kv_step_buf, q_buf, kv_buf, sems,
    ):
        copies = []

        def save(source, target):
            copy = pltpu.make_async_copy(source, target, sems.at[len(copies)])
            copy.start()
            copies.append(copy)

        q_width, model = q_buf.shape
        piece = model // PARTS
        sums = squares_0[...] + squares_1[...] + squares_2[...] + squares_3[...]
        q_scale = 0.5 * jnp.sqrt(F32(q_count)) * lax.rsqrt(sums[0:1, 0:1] + 1e-06)
        kv_scale = 0.5 * jnp.sqrt(F32(kv_count)) * lax.rsqrt(sums[1:2, 0:1] + 1e-06)
        own = own_ref[...]
        step = q_scale * own[:, :q_width]
        q_step_buf[...] = step
        q_new_buf[...] = q_ref[...] - step
        step = kv_scale * own[:, q_width:]
        kv_step_buf[...] = step
        kv_new_buf[...] = kv_ref[...] - step
        save(q_step_buf, q_step)
        save(q_new_buf, q_new)
        save(kv_step_buf, kv_step)
        save(kv_new_buf, kv_new)
        for p in range(PARTS):
            at = slice(p * piece, (p + 1) * piece)
            q_buf[:, at] = (q_whole_ref[:, at].astype(F32) - q_scale * q_step_ref[:, at]).astype(BF16)
            save(q_buf.at[:, at], q_copy.at[:, at])
        for p in range(PARTS):
            at = slice(p * piece, (p + 1) * piece)
            kv_buf[at] = (kv_whole_ref[at].astype(F32) - kv_scale * kv_step_ref[at]).astype(BF16)
            save(kv_buf.at[at], kv_copy.at[at])
        for copy in copies:
            copy.wait()

    return kernel


def finish(squares, q_steps, kv_steps, own, q_whole, kv_whole, q_own, kv_own, q_count, kv_count):
    made = [
        (q_own.shape, F32),
        (kv_own.shape, F32),
        (q_own.shape, F32),
        (kv_own.shape, F32),
        (q_whole.shape, BF16),
        (kv_whole.shape, BF16),
    ]
    return run(
        finish_kernel(q_count, kv_count),
        [VMEM] * 11,
        (*squares, q_steps, kv_steps, own, q_whole, kv_whole, q_own, kv_own),
        [far(*m) for m in made],
        [pltpu.VMEM(*m) for m in made] + [pltpu.SemaphoreType.DMA((4 + 2 * PARTS,))],
        outs=[HBM] * 6,
    )


def body(x, q_cot, kv_cot, row_factor, q_weight, kv_weight, qm, km, qs, ks):
    fs_count = lax.axis_size(FS)
    q_width, kv_width = q_cot.shape[1], kv_cot.shape[1]
    width, rank_rows = q_width + kv_width, qm.shape[0]
    chips = lax.axis_size(ZY)
    factor_tiles, weight_rows, moments = spread(
        row_factor, q_weight, kv_weight, qm, km, qs, ks, chips
    )
    weight_more = swapped(weight_rows, "core", 1)
    weight_across = shifted(weight_rows, "y", lax.axis_size("y") // 2)
    mine = exchange(factor_tiles, ZY)
    grad, weight_both = gradients(q_cot.T, kv_cot, x, weight_rows, weight_more)
    mine, grad, weight_both, weight_rows = lax.optimization_barrier(
        (mine, grad, weight_both, weight_rows)
    )
    other = swapped(mine, "core", 1)
    weight_beside = turned(weight_both, "y")
    partial, factor = project(mine, other, grad)
    parts = exchange(partial.reshape(fs_count, rank_rows, width), FS)
    weight_part = stacked((weight_rows, weight_beside, weight_across))
    weight_row = stacked((weight_part, swapped(weight_part, "core", 1)))
    weight_near = turned(weight_row, "z")
    to_send, sums = direction_tiles(parts, moments)
    directions = exchange(to_send, FS).reshape(fs_count * rank_rows, width)
    weight_over = swapped(weight_near, "core", 1)
    weight_far = shifted(weight_part, "z", lax.axis_size("z") // 2)
    weight_last = swapped(weight_far, "core", 1)
    q_whole, kv_whole = weights(
        (weight_row, weight_near, weight_over, weight_far, weight_last),
        lax.axis_size("z"), q_weight.shape[0], q_width, kv_width,
    )
    squares = stats(directions, q_width)
    squares = [squares] + [shifted(squares, "tp", k) for k in (2, 1, 3)]
    q_steps, kv_steps, own, *kept = unscaled_steps(
        directions, factor, row_factor, sums, moments, (qm, km, qs, ks)
    )
    count = rank_rows * fs_count * lax.axis_size("tp")
    q_new, kv_new, q_step, kv_step, q_copy, kv_copy = finish(
        squares, q_steps, kv_steps, own, q_whole, kv_whole, q_weight, kv_weight,
        count * q_width, count * kv_width,
    )
    return (q_new, kv_new, q_step, kv_step, q_copy.T, kv_copy, *kept)


def solution(mesh):
    split = Mesh(mesh.devices.reshape(4, 4, 2, mesh.shape["tp"]), ("z", "y", "core", "tp"))
    rows, tiles = P(FS, None), P(FS, "tp")
    return jax.shard_map(
        body,
        mesh=split,
        in_specs=(rows, tiles, tiles, rows, tiles, tiles, tiles, tiles, tiles, tiles),
        out_specs=(tiles, tiles, tiles, tiles, P(None, "tp"), P(None, "tp"), tiles, tiles, tiles, tiles),
        check_vma=False,
    )
```

```python
import jax
import jax.numpy as jnp
from jax import lax
from jax.experimental import pallas as pl
from jax.experimental.pallas import tpu as pltpu
from jax.sharding import Mesh
from jax.sharding import PartitionSpec as P


FS = ("z", "y", "core")
ZY = ("z", "y")
BF16 = jnp.bfloat16
F32 = jnp.float32
VMEM = pl.BlockSpec(memory_space=pltpu.MemorySpace.VMEM)
HBM = pl.BlockSpec(memory_space=pltpu.MemorySpace.HBM)
PLACES = {id(VMEM): pltpu.MemorySpace.VMEM, id(HBM): pltpu.MemorySpace.HBM}


def near(dims, kind=F32):
    return pltpu.MemorySpace.VMEM(dims, kind)


def far(dims, kind=F32):
    return jax.ShapeDtypeStruct(dims, kind)


def run(kernel, specs, operands, out, scratch=(), flops=0, limit=8, outs=None):
    operands = [
        pltpu.with_memory_space_constraint(o, PLACES[id(s)]) if id(s) in PLACES else o
        for s, o in zip(specs, operands)
    ]
    return pl.pallas_call(
        kernel,
        in_specs=list(specs),
        out_specs=outs or [VMEM] * len(out),
        out_shape=list(out),
        scratch_shapes=list(scratch),
        compiler_params=pltpu.CompilerParams(vmem_limit_bytes=limit * 1024 * 1024),
        cost_estimate=pl.CostEstimate(flops=flops, bytes_accessed=0, transcendentals=0),
    )(*operands)


def exchange(tiles, axis):
    return lax.all_to_all(tiles, axis, split_axis=0, concat_axis=0, tiled=True)


def swapped(array, axis, bit):
    count = lax.axis_size(axis)
    return lax.ppermute(array, axis, [(i, i ^ bit) for i in range(count)])


def shifted(array, axis, k):
    count = lax.axis_size(axis)
    return lax.ppermute(array, axis, [(i, (i + k) % count) for i in range(count)])


def turned(array, axis):
    sizes = [lax.axis_size(a) for a in FS]
    at = FS.index(axis)
    pairs = []
    for z in range(sizes[0]):
        for y in range(sizes[1]):
            for core in range(sizes[2]):
                here, there = [z, y, core], [z, y, core]
                there[at] = (there[at] + 2 * core - 1) % sizes[at]
                pairs.append(
                    tuple((p[0] * sizes[1] + p[1]) * sizes[2] + p[2] for p in (here, there))
                )
    return lax.ppermute(array, FS, pairs)


LANES = 128
HALF = LANES // 2


def spread_kernel(
    factor_ref, q_ref, kv_ref, qm_ref, km_ref, qs_ref, ks_ref, factor_out, rows_out, moments_out,
    factor_buf, q_buf, kv_buf, qm_buf, km_buf, qs_buf, ks_buf, sems,
):
    pairs = (
        (factor_ref, factor_buf),
        (q_ref, q_buf),
        (kv_ref, kv_buf),
        (qm_ref, qm_buf),
        (km_ref, km_buf),
        (qs_ref, qs_buf),
        (ks_ref, ks_buf),
    )
    arrivals = [pltpu.make_async_copy(a, b, sems.at[i]) for i, (a, b) in enumerate(pairs)]
    for copy in arrivals:
        copy.start()
    arrivals[0].wait()
    sent = [
        pltpu.make_async_copy(factor_buf, factor_out.at[i], sems.at[len(pairs) + i])
        for i in range(factor_out.shape[0])
    ]
    for copy in sent:
        copy.start()
    for copy in arrivals[1:]:
        copy.wait()
    q_width = q_ref.shape[1]
    moments_out[0, :, :q_width] = qm_buf[...]
    moments_out[0, :, q_width:] = km_buf[...]
    moments_out[1, :, :q_width] = qs_buf[...]
    moments_out[1, :, q_width:] = ks_buf[...]
    rows = q_ref.shape[0]
    quarter = rows // 4
    q = q_buf[...].astype(BF16)
    rows_out[0, :rows, :LANES] = q[:, :LANES]
    rows_out[0, :rows, LANES:] = kv_buf[...].astype(BF16)
    for g in range(4):
        rows_out[0, rows:, HALF * g : HALF * (g + 1)] = q[quarter * g : quarter * (g + 1), LANES:]
    for copy in sent:
        copy.wait()


def spread(factor, q, kv, qm, km, qs, ks, count):
    rows, width = q.shape[0], q.shape[1] + kv.shape[1]
    operands = (factor, q, kv, qm, km, qs, ks)
    return run(
        spread_kernel,
        [HBM] * 7,
        operands,
        [
            far((count, *factor.shape), BF16),
            near((1, rows + rows // 4, 2 * LANES), BF16),
            near((2, qm.shape[0], width)),
        ],
        [pltpu.VMEM(o.shape, o.dtype) for o in operands] + [pltpu.SemaphoreType.DMA((7 + count,))],
        outs=[HBM, VMEM, VMEM],
    )


def stack_kernel(*refs):
    at = 0
    for ref in refs[:-1]:
        count = ref.shape[0]
        refs[-1][at : at + count] = ref[...]
        at += count


def stacked(tiles):
    count = sum(t.shape[0] for t in tiles)
    return run(
        stack_kernel, [VMEM] * len(tiles), tiles, [near((count, *tiles[0].shape[1:]), BF16)]
    )[0]


def gradient_kernel(
    q_ref, kv_ref, x_ref, rows_ref, more_ref, out_ref, both_ref, sum_ref, q_buf, kv_buf, x_buf, sems
):
    depth, block, _ = x_buf.shape
    steps = x_ref.shape[0] // block

    def copies(k):
        at, slot = pl.ds(k * block, block), k % depth
        return (
            pltpu.make_async_copy(q_ref.at[:, at], q_buf.at[slot], sems.at[slot, 0]),
            pltpu.make_async_copy(kv_ref.at[at, :], kv_buf.at[slot], sems.at[slot, 1]),
            pltpu.make_async_copy(x_ref.at[at, :], x_buf.at[slot], sems.at[slot, 2]),
        )

    for k in range(depth):
        for copy in copies(k):
            copy.start()
    both_ref[0] = rows_ref[0]
    both_ref[1] = more_ref[0]
    for k in range(steps):
        slot = k % depth
        for copy in copies(k):
            copy.wait()
        left = jnp.concatenate([q_buf[slot], kv_buf[slot].T], axis=0)
        piece = jnp.dot(left, x_buf[slot], preferred_element_type=F32)
        if k == 0:
            sum_ref[...] = piece
        elif k < steps - 1:
            sum_ref[...] += piece
        else:
            out_ref[...] = (sum_ref[...] + piece).astype(BF16)
        if k + depth < steps:
            for copy in copies(k + depth):
                copy.start()


def gradients(q_turned, kv, x, rows, more, block=512, depth=4):
    q_width, kv_width = q_turned.shape[0], kv.shape[1]
    width = q_width + kv_width
    tokens, model = x.shape
    return run(
        gradient_kernel,
        [HBM] * 3 + [VMEM] * 2,
        (q_turned, kv, x, rows, more),
        [near((width, model), BF16), near((2, *rows.shape[1:]), BF16)],
        [
            pltpu.VMEM((width, model), F32),
            pltpu.VMEM((depth, q_width, block), BF16),
            pltpu.VMEM((depth, block, kv_width), BF16),
            pltpu.VMEM((depth, block, model), BF16),
            pltpu.SemaphoreType.DMA((depth, 3)),
        ],
        2 * width * tokens * model,
        24,
    )


def project_kernel(mine_ref, other_ref, grad_ref, out_ref, factor_ref):
    core = lax.axis_index("core")
    count, pair, rows, rank = factor_ref.shape
    for i in range(count):
        factor_ref[i, core] = mine_ref[i]
        factor_ref[i, 1 - core] = other_ref[i]
    factor = factor_ref[...].reshape(count * pair * rows, rank)
    out_ref[...] = jnp.dot(grad_ref[...], factor, preferred_element_type=F32).T.astype(BF16)


def project(mine, other, grad):
    count, rows, rank = mine.shape
    partial, factor = run(
        project_kernel,
        [VMEM] * 3,
        (mine, other, grad),
        [near((rank, grad.shape[0]), BF16), near((count, 2, rows, rank), BF16)],
    )
    return partial, factor.reshape(count * 2 * rows, rank)


def update(value, first, second):
    return 0.8 * first + 0.2 * value, 0.9 * second + 0.1 * value * value


def direction_kernel(parts_ref, moments_ref, out_ref, sums_ref):
    value = jnp.sum(parts_ref[...].astype(F32), axis=0)
    sums_ref[...] = value
    first, second = update(value, moments_ref[0], moments_ref[1])
    direction = (first / (jnp.sqrt(second) + 1e-08)).astype(BF16)
    for i in range(out_ref.shape[0]):
        out_ref[i] = direction


def direction_tiles(parts, moments):
    return run(
        direction_kernel,
        [VMEM] * 2,
        (parts, moments),
        [near(parts.shape, BF16), near(parts.shape[1:])],
    )


def stats_kernel(q_width):
    def kernel(dir_ref, out_ref):
        values = dir_ref[...].astype(F32)
        squares = jnp.sum(values * values, axis=0, keepdims=True)
        out_ref[0:1, :] = jnp.broadcast_to(jnp.sum(squares[:, :q_width], axis=1, keepdims=True), (1, 128))
        out_ref[1:2, :] = jnp.broadcast_to(jnp.sum(squares[:, q_width:], axis=1, keepdims=True), (1, 128))
        out_ref[2:, :] = jnp.zeros((6, 128), F32)

    return kernel


def stats(directions, q_width):
    return run(stats_kernel(q_width), [VMEM], (directions,), [near((8, 128))])[0]


def weights_kernel(here_ref, near_ref, over_ref, far_ref, last_ref, q_ref, kv_ref, first_ref, rest_ref):
    z, y, core = (lax.axis_index(a) for a in FS)
    count, _, _, rows, _ = first_ref.shape
    quarter = rows // 4
    turn = 2 * core - 1

    def around(value):
        return lax.rem(value + count, count)

    def pieces(c):
        t = 2 * c - 1
        return [(y, c), (around(y - t), c), (around(y - t), 1 - c), (around(y + count // 2), c)]

    mine, other = pieces(core), pieces(1 - core)
    for ref, zi, order in (
        (here_ref, z, mine + other),
        (near_ref, around(z - turn), mine + other),
        (over_ref, around(z + turn), other + mine),
        (far_ref, around(z + count // 2), mine),
        (last_ref, around(z + count // 2), other),
    ):
        for k, (yi, c) in enumerate(order):
            first_ref[zi, yi, c] = ref[k, :rows, :LANES]
            kv_ref[zi, yi, c] = ref[k, :rows, LANES:]
            for g in range(4):
                rest_ref[zi, yi, c, quarter * g : quarter * (g + 1), :HALF] = ref[
                    k, rows:, HALF * g : HALF * (g + 1)
                ]
    model = q_ref.shape[1]
    q_ref[:LANES] = first_ref[...].reshape(model, LANES).T
    q_ref[LANES:] = rest_ref[...].reshape(model, LANES).T[:HALF]


def weights(pieces, count, rows, q_width, kv_width):
    blocks = (count, count, 2, rows)
    model = count * count * 2 * rows
    q_turned, kv = run(
        weights_kernel,
        [VMEM] * len(pieces),
        pieces,
        [near((q_width, model), BF16), near((*blocks, kv_width), BF16)],
        [pltpu.VMEM((*blocks, LANES), BF16), pltpu.VMEM((*blocks, LANES), BF16)],
    )
    return q_turned, kv.reshape(model, kv_width)


NT = (((1,), (1,)), ((), ()))


def steps_kernel(
    dir_ref, factor_ref, own_ref, sums_ref, moments_ref,
    q_ref, kv_ref, own_out, qm_out, km_out, qs_out, ks_out, qm_buf, km_buf, qs_buf, ks_buf, sems,
):
    q_width = qm_buf.shape[1]
    first, second = update(sums_ref[...], moments_ref[0], moments_ref[1])
    qm_buf[...] = first[:, :q_width]
    km_buf[...] = first[:, q_width:]
    qs_buf[...] = second[:, :q_width]
    ks_buf[...] = second[:, q_width:]
    saved = [
        pltpu.make_async_copy(a, b, sems.at[i])
        for i, (a, b) in enumerate(
            ((qm_buf, qm_out), (km_buf, km_out), (qs_buf, qs_out), (ks_buf, ks_out))
        )
    ]
    for copy in saved:
        copy.start()
    directions = dir_ref[...]
    factor = factor_ref[...]
    turned = directions[:, :q_width].T
    q_ref[...] = lax.dot_general(turned, factor, NT, preferred_element_type=F32)
    kv_ref[...] = jnp.dot(factor, directions[:, q_width:], preferred_element_type=F32)
    own_out[...] = jnp.dot(own_ref[...], directions, preferred_element_type=F32)
    for copy in saved:
        copy.wait()


def unscaled_steps(directions, factor, own, sums, moments, kept):
    model, width = factor.shape[0], directions.shape[1]
    q_width = kept[0].shape[1]
    return run(
        steps_kernel,
        [VMEM] * 5,
        (directions, factor, own, sums, moments),
        [near((q_width, model)), near((model, width - q_width)), near((own.shape[0], width))]
        + [far(k.shape) for k in kept],
        [pltpu.VMEM(k.shape, F32) for k in kept] + [pltpu.SemaphoreType.DMA((len(kept),))],
        2 * width * directions.shape[0] * model,
        outs=[VMEM] * 3 + [HBM] * 4,
    )


PARTS = 2


def finish_kernel(q_count, kv_count):
    def kernel(
        squares_0, squares_1, squares_2, squares_3, q_step_ref, kv_step_ref, own_ref, q_whole_ref,
        kv_whole_ref, q_ref, kv_ref, q_new, kv_new, q_step, kv_step, q_copy, kv_copy,
        q_new_buf, kv_new_buf, q_step_buf, kv_step_buf, q_buf, kv_buf, sems,
    ):
        copies = []

        def save(source, target):
            copy = pltpu.make_async_copy(source, target, sems.at[len(copies)])
            copy.start()
            copies.append(copy)

        q_width, model = q_buf.shape
        piece = model // PARTS
        sums = squares_0[...] + squares_1[...] + squares_2[...] + squares_3[...]
        q_scale = 0.5 * jnp.sqrt(F32(q_count)) * lax.rsqrt(sums[0:1, 0:1] + 1e-06)
        kv_scale = 0.5 * jnp.sqrt(F32(kv_count)) * lax.rsqrt(sums[1:2, 0:1] + 1e-06)
        own = own_ref[...]
        step = q_scale * own[:, :q_width]
        q_step_buf[...] = step
        q_new_buf[...] = q_ref[...] - step
        step = kv_scale * own[:, q_width:]
        kv_step_buf[...] = step
        kv_new_buf[...] = kv_ref[...] - step
        save(q_step_buf, q_step)
        save(q_new_buf, q_new)
        save(kv_step_buf, kv_step)
        save(kv_new_buf, kv_new)
        for p in range(PARTS):
            at = slice(p * piece, (p + 1) * piece)
            q_buf[:, at] = (q_whole_ref[:, at].astype(F32) - q_scale * q_step_ref[:, at]).astype(BF16)
            save(q_buf.at[:, at], q_copy.at[:, at])
        for p in range(PARTS):
            at = slice(p * piece, (p + 1) * piece)
            kv_buf[at] = (kv_whole_ref[at].astype(F32) - kv_scale * kv_step_ref[at]).astype(BF16)
            save(kv_buf.at[at], kv_copy.at[at])
        for copy in copies:
            copy.wait()

    return kernel


def finish(squares, q_steps, kv_steps, own, q_whole, kv_whole, q_own, kv_own, q_count, kv_count):
    made = [
        (q_own.shape, F32),
        (kv_own.shape, F32),
        (q_own.shape, F32),
        (kv_own.shape, F32),
        (q_whole.shape, BF16),
        (kv_whole.shape, BF16),
    ]
    return run(
        finish_kernel(q_count, kv_count),
        [VMEM] * 11,
        (*squares, q_steps, kv_steps, own, q_whole, kv_whole, q_own, kv_own),
        [far(*m) for m in made],
        [pltpu.VMEM(*m) for m in made] + [pltpu.SemaphoreType.DMA((4 + 2 * PARTS,))],
        outs=[HBM] * 6,
    )


def body(x, q_cot, kv_cot, row_factor, q_weight, kv_weight, qm, km, qs, ks):
    fs_count = lax.axis_size(FS)
    q_width, kv_width = q_cot.shape[1], kv_cot.shape[1]
    width, rank_rows = q_width + kv_width, qm.shape[0]
    chips = lax.axis_size(ZY)
    factor_tiles, weight_rows, moments = spread(
        row_factor, q_weight, kv_weight, qm, km, qs, ks, chips
    )
    weight_more = swapped(weight_rows, "core", 1)
    weight_across = shifted(weight_rows, "y", lax.axis_size("y") // 2)
    mine = exchange(factor_tiles, ZY)
    grad, weight_both = gradients(q_cot.T, kv_cot, x, weight_rows, weight_more)
    mine, grad, weight_both, weight_rows = lax.optimization_barrier(
        (mine, grad, weight_both, weight_rows)
    )
    other = swapped(mine, "core", 1)
    weight_beside = turned(weight_both, "y")
    partial, factor = project(mine, other, grad)
    parts = exchange(partial.reshape(fs_count, rank_rows, width), FS)
    weight_part = stacked((weight_rows, weight_beside, weight_across))
    weight_row = stacked((weight_part, swapped(weight_part, "core", 1)))
    weight_near = turned(weight_row, "z")
    to_send, sums = direction_tiles(parts, moments)
    directions = exchange(to_send, FS).reshape(fs_count * rank_rows, width)
    weight_over = swapped(weight_near, "core", 1)
    weight_far = shifted(weight_part, "z", lax.axis_size("z") // 2)
    weight_last = swapped(weight_far, "core", 1)
    q_whole, kv_whole = weights(
        (weight_row, weight_near, weight_over, weight_far, weight_last),
        lax.axis_size("z"), q_weight.shape[0], q_width, kv_width,
    )
    squares = stats(directions, q_width)
    squares = [squares] + [shifted(squares, "tp", k) for k in (2, 1, 3)]
    q_steps, kv_steps, own, *kept = unscaled_steps(
        directions, factor, row_factor, sums, moments, (qm, km, qs, ks)
    )
    count = rank_rows * fs_count * lax.axis_size("tp")
    q_new, kv_new, q_step, kv_step, q_copy, kv_copy = finish(
        squares, q_steps, kv_steps, own, q_whole, kv_whole, q_weight, kv_weight,
        count * q_width, count * kv_width,
    )
    return (q_new, kv_new, q_step, kv_step, q_copy.T, kv_copy, *kept)


def solution(mesh):
    split = Mesh(mesh.devices.reshape(4, 4, 2, mesh.shape["tp"]), ("z", "y", "core", "tp"))
    rows, tiles = P(FS, None), P(FS, "tp")
    return jax.shard_map(
        body,
        mesh=split,
        in_specs=(rows, tiles, tiles, rows, tiles, tiles, tiles, tiles, tiles, tiles),
        out_specs=(tiles, tiles, tiles, tiles, P(None, "tp"), P(None, "tp"), tiles, tiles, tiles, tiles),
        check_vma=False,
    )
```
